32 devices in a mesh: sp: 16 (over z, y, x), tp: 2 (over core).
Axes of the slice: x: 2, y: 2, z: 4, core: 2. Of those that a mesh axis runs over, the one named last changes fastest.
Arguments:
- hidden_in: bfloat16 [4096, 2048], P('sp', 'tp'), may hold values from -6 to 6
- w_query_rec: bfloat16 [2048, 2048], P('sp', 'tp'), may hold values from -0.125 to 0.125
- w_forget: bfloat16 [2048, 2048], P('sp', 'tp'), may hold values from -0.125 to 0.125
- w_input: bfloat16 [2048, 2048], P('sp', 'tp'), may hold values from -0.125 to 0.125
- forget_gap: float32 [2048], P('tp'), may hold values from 1e-05 to 0.08
- decay_extra: float32 [4096, 16], P('sp', 'tp'), may hold values from -0.75 to 0
- rec_gain: float32 [128], replicated, may hold values from 0.1 to 1.9
- w_q_down: bfloat16 [2048, 512], P(None, 'tp'), may hold values from -0.125 to 0.125
- w_kv_down: bfloat16 [2048, 256], P(None, 'tp'), may hold values from -0.125 to 0.125
- w_key_rope: bfloat16 [2048, 32], replicated, may hold values from -0.125 to 0.125
- q_gain: float32 [512], replicated, may hold values from 1.4 to 7
- kv_gain: float32 [256], replicated, may hold values from 1.4 to 7
- w_q_nope: bfloat16 [512, 1024], P(None, 'tp'), may hold values from -0.25 to 0.25
- w_q_rope: bfloat16 [512, 512], P(None, 'tp'), may hold values from -0.25 to 0.25
- w_k_up: bfloat16 [256, 1024], P(None, 'tp'), may hold values from -0.375 to 0.375
- w_v_up: bfloat16 [256, 1024], P(None, 'tp'), may hold values from -0.375 to 0.375
- w_out_rec: bfloat16 [2048, 2048], P('tp'), may hold values from -0.109375 to 0.109375
- w_out_att: bfloat16 [1024, 2048], P('tp'), may hold values from -0.109375 to 0.109375
Outputs:
- mixed_out: bfloat16 [4096, 2048], P(('sp', 'tp'))
The draws below stay inside these ranges and needn't reach their ends.
All inputs are finite; a program needn't handle non-finite values.
Results may differ from the reference program's by a relative error of at most 0.02.
The reference program's roundings to bfloat16 on the way count: a program that leaves them out, or rounds other values in their place, can miss the bound.
Values may be sent and summed in bfloat16 or wider, within the bound.
A program may use at most 128 MiB of HBM per device.

```python
import math
import jax
import jax.numpy as jnp
from jax import lax

D = 2048
RECURRENT_HEADS = 16
HG_KDIM = 128
HG_VDIM = 128
HG_BLOCK = 64
MLA_HEADS = 16
NOPE = 64
ROPE = 32
MLA_V = 64
Q_RANK = 512
KV_RANK = 256
TOK_DEV = 256
SEQUENCE_TOKENS = 4096


def draw_forget_gap(key, part):
    first_key, key_second_draw, key_third_draw = jax.random.split(jax.random.fold_in(key, 11), 3)
    fast_share = 0.5
    fast_heads = jax.random.uniform(first_key, (RECURRENT_HEADS, 1)) < fast_share
    slow_gap = jnp.exp(jax.random.uniform(key_second_draw, (RECURRENT_HEADS, HG_KDIM), jnp.float32, jnp.log(1e-05), jnp.log(0.0001)))
    fast_gap = jnp.exp(jax.random.uniform(key_third_draw, (RECURRENT_HEADS, HG_KDIM), jnp.float32, jnp.log(0.03), jnp.log(0.08)))
    return jnp.where(fast_heads, fast_gap, slow_gap).reshape(RECURRENT_HEADS * HG_KDIM).astype(jnp.float32)


def draw_decay_extra(key, part):
    first_key, key_second_draw, key_third_draw = jax.random.split(jax.random.fold_in(key, 23), 3)
    block_count = SEQUENCE_TOKENS // TOK_DEV
    forget_base_rate = jnp.exp(jax.random.uniform(first_key, (block_count, 1, RECURRENT_HEADS), jnp.float32, jnp.log(0.2), 0.0)) / SEQUENCE_TOKENS
    forget_base_rate = jnp.broadcast_to(forget_base_rate, (block_count, TOK_DEV, RECURRENT_HEADS)).reshape(SEQUENCE_TOKENS, RECURRENT_HEADS)
    spike_events = jax.random.uniform(key_second_draw, (SEQUENCE_TOKENS, RECURRENT_HEADS)) < 3.0 / SEQUENCE_TOKENS
    spike_depth = jax.random.uniform(key_third_draw, (SEQUENCE_TOKENS, RECURRENT_HEADS), jnp.float32, jnp.log(0.5), jnp.log(0.8))
    return (jnp.where(spike_events, spike_depth, 0.0) - forget_base_rate).astype(jnp.float32)


def draw_q_gain(key, part):
    values = jax.random.uniform(jax.random.fold_in(key, 31), (Q_RANK,), jnp.float32, 1.4, 2.6)
    return values.astype(jnp.float32)


def draw_kv_gain(key, part):
    values = jax.random.uniform(jax.random.fold_in(key, 37), (KV_RANK,), jnp.float32, 1.4, 2.6)
    return values.astype(jnp.float32)


def level_of(key, dims, shards, low, high):
    def one(dim, parts):
        heights = jax.random.uniform(jax.random.fold_in(jax.random.fold_in(key, 6), dim), (parts,), jnp.float32, low / len(shards), high / len(shards))
        return jnp.repeat(jnp.exp(heights), dims[dim] // parts).reshape((-1,) + (1,) * (len(dims) - dim - 1))

    loudness = one(*shards[0])
    for cut in shards[1:]:
        loudness = loudness * one(*cut)
    return loudness


def scatter_about(key, dims, deviation, bound, cuts=(), kind=jnp.bfloat16):
    drawn = deviation * jax.random.normal(key, dims, jnp.float32)
    if cuts:
        drawn = drawn * level_of(key, dims, cuts, -0.22, 0.18)
    return jnp.clip(drawn, -bound, bound).astype(kind)


def setup_inputs(seed: int = 0) -> dict:
    arg_keys = jax.random.split(jax.random.key(seed), 19)
    return {
        "hidden_in": scatter_about(arg_keys[0], (SEQUENCE_TOKENS, D), 1.0, 6.0, ((0, 16), (1, 2))),
        "w_query_rec": scatter_about(arg_keys[1], (D, RECURRENT_HEADS * HG_KDIM), D ** -0.5, 0.125, ((0, 16), (1, 2))),
        "w_forget": scatter_about(arg_keys[2], (D, RECURRENT_HEADS * HG_KDIM), D ** -0.5, 0.125, ((0, 16), (1, 2))),
        "w_input": scatter_about(arg_keys[3], (D, RECURRENT_HEADS * HG_VDIM), D ** -0.5, 0.125, ((0, 16), (1, 2))),
        "forget_gap": draw_forget_gap(jax.random.fold_in(arg_keys[18], 71), 0),
        "decay_extra": draw_decay_extra(jax.random.fold_in(arg_keys[18], 71), 0),
        "rec_gain": jnp.clip(1.0 + 0.18 * jax.random.normal(arg_keys[6], (HG_VDIM,), jnp.float32), 0.1, 1.9),
        "w_q_down": scatter_about(arg_keys[7], (D, Q_RANK), D ** -0.5, 0.125, ((1, 2),)),
        "w_kv_down": scatter_about(arg_keys[8], (D, KV_RANK), D ** -0.5, 0.125, ((1, 2),)),
        "w_key_rope": scatter_about(arg_keys[9], (D, ROPE), D ** -0.5, 0.125),
        "q_gain": draw_q_gain(jax.random.fold_in(arg_keys[18], 71), 0),
        "kv_gain": draw_kv_gain(jax.random.fold_in(arg_keys[18], 71), 0),
        "w_q_nope": scatter_about(arg_keys[12], (Q_RANK, MLA_HEADS * NOPE), Q_RANK ** -0.5, 0.25, ((1, 2),)),
        "w_q_rope": scatter_about(arg_keys[13], (Q_RANK, MLA_HEADS * ROPE), Q_RANK ** -0.5, 0.25, ((1, 2),)),
        "w_k_up": scatter_about(arg_keys[14], (KV_RANK, MLA_HEADS * NOPE), KV_RANK ** -0.5, 0.375, ((1, 2),)),
        "w_v_up": scatter_about(arg_keys[15], (KV_RANK, MLA_HEADS * MLA_V), KV_RANK ** -0.5, 0.375, ((1, 2),)),
        "w_out_rec": scatter_about(arg_keys[16], (RECURRENT_HEADS * HG_VDIM, D), (RECURRENT_HEADS * HG_VDIM + MLA_HEADS * MLA_V) ** -0.5, 0.109375, ((0, 2),)),
        "w_out_att": scatter_about(arg_keys[17], (MLA_HEADS * MLA_V, D), (RECURRENT_HEADS * HG_VDIM + MLA_HEADS * MLA_V) ** -0.5, 0.109375, ((0, 2),)),
    }


NORM_EPS = 1e-06
ROPE_BASE = 10000.0
NEG_BIG = -1e+30

def rms_scale(values):
    return values * lax.rsqrt(lax.optimization_barrier(jnp.mean(values * values, axis=-1, keepdims=True)) + NORM_EPS)

def rotate_half(values, cosine, sine_table):
    half_width = values.shape[-1] // 2
    lower_half = values[..., :half_width]
    upper_half = values[..., half_width:]
    return jnp.concatenate([lower_half * cosine - upper_half * sine_table, lower_half * sine_table + upper_half * cosine], axis=-1)

def rotary_tables(row_count, offset, rot_width):
    positions = jnp.arange(row_count, dtype=jnp.float32) + offset
    frequency = 1.0 / ROPE_BASE ** (jnp.arange(0, rot_width, 2, dtype=jnp.float32) / rot_width)
    angles = positions[:, None] * frequency[None, :]
    return (jnp.cos(angles), jnp.sin(angles))

def block_step(rec_state, inputs):
    queries, key_in, values, log_forget = inputs
    cumulative = jnp.cumsum(log_forget, axis=1)
    log_gaps = cumulative[:, :, None, :] - cumulative[:, None, :, :]
    block_len = queries.shape[1]
    lower_mask = jnp.tril(jnp.ones((block_len, block_len), jnp.float32))
    decays = jnp.exp(jnp.minimum(log_gaps, 0.0)) * lower_mask[None, :, :, None]
    scores = jnp.einsum('htsd,hsd->hts', queries[:, :, None, :] * decays, key_in, precision=lax.Precision.HIGHEST)
    block_out = jnp.einsum('hts,hsv->htv', scores, values, precision=lax.Precision.HIGHEST) + jnp.einsum('htd,hdv->htv', queries * jnp.exp(cumulative), rec_state, precision=lax.Precision.HIGHEST)
    last_cumul = cumulative[:, -1:, :]
    rec_state = jnp.exp(last_cumul[:, 0, :])[..., None] * rec_state + jnp.einsum('hsd,hsv->hdv', key_in * jnp.exp(last_cumul - cumulative), values, precision=lax.Precision.HIGHEST)
    return (rec_state, block_out)

def recurrence(queries, key_in, values, log_forget):
    seq_total, head_count, key_width = queries.shape
    block_count = seq_total // HG_BLOCK

    def to_blocks(tensor):
        return tensor.reshape(block_count, HG_BLOCK, head_count, tensor.shape[-1]).transpose(0, 2, 1, 3)
    initial = jnp.zeros((head_count, key_width, values.shape[-1]), jnp.float32)
    _, outputs = lax.scan(block_step, initial, (to_blocks(queries), to_blocks(key_in), to_blocks(values), to_blocks(log_forget)))
    return outputs.transpose(0, 2, 1, 3).reshape(seq_total, head_count, values.shape[-1])

def score_block(q_nope, q_rope, k_nope, k_rope, values, q_start, k_start):
    score_scale = 1.0 / math.sqrt(NOPE + ROPE)
    scores = (jnp.einsum('qhd,khd->hqk', q_nope.astype(jnp.float32), k_nope.astype(jnp.float32)) + jnp.einsum('qhr,kr->hqk', q_rope.astype(jnp.float32), k_rope.astype(jnp.float32))) * score_scale
    q_pos = q_start + jnp.arange(q_nope.shape[0], dtype=jnp.int32)
    k_pos = k_start + jnp.arange(k_nope.shape[0], dtype=jnp.int32)
    allowed = k_pos[None, :] <= q_pos[:, None]
    scores = jnp.where(allowed[None], scores, NEG_BIG)
    block_peak = lax.optimization_barrier(jnp.max(scores, axis=-1))
    weights = jnp.where(allowed[None], jnp.exp(scores - block_peak[..., None]), 0.0)
    block_total = lax.optimization_barrier(jnp.sum(weights, axis=-1))
    weights16 = weights.astype(jnp.bfloat16)
    block_sum = jnp.einsum('hqk,khv->hqv', weights16.astype(jnp.float32), values.astype(jnp.float32))
    return (block_peak, block_total, block_sum)

def merge_terms(earlier, later_part):
    top = jnp.maximum(earlier[0], later_part[0])
    old_factor = jnp.exp(earlier[0] - top)
    new_factor = jnp.exp(later_part[0] - top)
    return (top, earlier[1] * old_factor + later_part[1] * new_factor, earlier[2] * old_factor[..., None] + later_part[2] * new_factor[..., None])

def reference(hidden_in, w_query_rec, w_forget, w_input, forget_gap, decay_extra, rec_gain, w_q_down, w_kv_down, w_key_rope, q_gain, kv_gain, w_q_nope, w_q_rope, w_k_up, w_v_up, w_out_rec, w_out_att):
    seq_total = hidden_in.shape[0]

    def project_input(weight):
        return jnp.dot(hidden_in, weight, preferred_element_type=jnp.float32).astype(jnp.bfloat16)
    rec_query = project_input(w_query_rec).astype(jnp.float32).reshape(seq_total, RECURRENT_HEADS, HG_KDIM)
    forget_pre = project_input(w_forget).astype(jnp.float32).reshape(seq_total, RECURRENT_HEADS, HG_KDIM)
    rec_value = project_input(w_input).astype(jnp.float32).reshape(seq_total, RECURRENT_HEADS, HG_VDIM)
    gap_rows = forget_gap.reshape(RECURRENT_HEADS, HG_KDIM)
    closing = jax.nn.sigmoid(-forget_pre)
    key_in = gap_rows * closing
    log_forget = jnp.log1p(-gap_rows * closing) + decay_extra[:, :, None]
    rec_raw = recurrence(rec_query, key_in, rec_value, log_forget)
    rec_out = (rms_scale(rec_raw) * rec_gain).astype(jnp.bfloat16).reshape(seq_total, RECURRENT_HEADS * HG_VDIM)
    q_latent = project_input(w_q_down)
    kv_latent = project_input(w_kv_down)
    q_normed = (rms_scale(q_latent.astype(jnp.float32)) * q_gain).astype(jnp.bfloat16)
    latent = (rms_scale(kv_latent.astype(jnp.float32)) * kv_gain).astype(jnp.bfloat16)
    cosine, sine_table = rotary_tables(seq_total, 0.0, ROPE)
    key_rope = rotate_half(jnp.dot(hidden_in, w_key_rope, preferred_element_type=jnp.float32), cosine, sine_table).astype(jnp.bfloat16)
    q_nope = jnp.dot(q_normed, w_q_nope, preferred_element_type=jnp.float32).astype(jnp.bfloat16)
    q_nope = q_nope.reshape(seq_total, MLA_HEADS, NOPE)
    q_rope = jnp.dot(q_normed, w_q_rope, preferred_element_type=jnp.float32).reshape(seq_total, MLA_HEADS, ROPE)
    q_rope = rotate_half(q_rope, cosine[:, None, :], sine_table[:, None, :]).astype(jnp.bfloat16)
    k_nope = jnp.dot(latent, w_k_up, preferred_element_type=jnp.float32).astype(jnp.bfloat16)
    k_nope = k_nope.reshape(seq_total, MLA_HEADS, NOPE)
    att_value = jnp.dot(latent, w_v_up, preferred_element_type=jnp.float32).astype(jnp.bfloat16)
    att_value = att_value.reshape(seq_total, MLA_HEADS, MLA_V)
    block_len = TOK_DEV
    block_count = seq_total // block_len

    def per_query(query_block):
        q_start = (query_block * block_len).astype(jnp.int32)
        query_nope = lax.dynamic_slice_in_dim(q_nope, q_start, block_len, 0)
        query_rope = lax.dynamic_slice_in_dim(q_rope, q_start, block_len, 0)

        def inner(key_block, running):
            k_start = (key_block * block_len).astype(jnp.int32)
            partials = score_block(query_nope, query_rope, lax.dynamic_slice_in_dim(k_nope, k_start, block_len, 0), lax.dynamic_slice_in_dim(key_rope, k_start, block_len, 0), lax.dynamic_slice_in_dim(att_value, k_start, block_len, 0), q_start, k_start)
            return merge_terms(running, partials)
        initial = (jnp.full((MLA_HEADS, block_len), NEG_BIG, jnp.float32), jnp.zeros((MLA_HEADS, block_len), jnp.float32), jnp.zeros((MLA_HEADS, block_len, MLA_V), jnp.float32))
        top, total_w, accum = lax.fori_loop(jnp.int32(0), query_block + 1, inner, initial)
        result = accum / total_w[..., None]
        return result.transpose(1, 0, 2).reshape(block_len, MLA_HEADS * MLA_V).astype(jnp.bfloat16)
    att_out = lax.map(per_query, jnp.arange(block_count, dtype=jnp.int32)).reshape(seq_total, MLA_HEADS * MLA_V)
    mixed_out = jnp.dot(rec_out, w_out_rec, preferred_element_type=jnp.float32) + jnp.dot(att_out, w_out_att, preferred_element_type=jnp.float32)
    return mixed_out.astype(jnp.bfloat16)
```

```python
import math

import jax
import jax.numpy as jnp
from jax import lax
from jax.experimental import pallas as pl
from jax.experimental.pallas import tpu as pltpu
from jax.sharding import Mesh
from jax.sharding import PartitionSpec as P

HG_KDIM = 128
HG_VDIM = 128
HG_BLOCK = 64
NOPE = 64
ROPE = 32
MLA_V = 64


NORM_EPS = 1e-06
ROPE_BASE = 10000.0
NEG_BIG = -1e30


def rotate_half(values, cosine, sine_table):
    half_width = values.shape[-1] // 2
    lower_half = values[..., :half_width]
    upper_half = values[..., half_width:]
    return jnp.concatenate(
        [
            lower_half * cosine - upper_half * sine_table,
            lower_half * sine_table + upper_half * cosine,
        ],
        axis=-1,
    )


def rotary_tables(row_count, offset, rot_width):
    positions = jnp.arange(row_count, dtype=jnp.float32) + offset
    frequency = 1.0 / ROPE_BASE ** (jnp.arange(0, rot_width, 2, dtype=jnp.float32) / rot_width)
    angles = positions[:, None] * frequency[None, :]
    return (jnp.cos(angles), jnp.sin(angles))


def dot_t(left, right, left_dim, right_dim):
    return lax.dot_general(
        left, right, (((left_dim,), (right_dim,)), ((), ())), preferred_element_type=jnp.float32
    )


def recurrence_body(rows, q_ref, k_ref, v_ref, lf_ref, s_ref, gain_ref, out_ref, state_ref):
    row_id = lax.broadcasted_iota(jnp.int32, (rows, rows), 0)
    col_id = lax.broadcasted_iota(jnp.int32, (rows, rows), 1)
    lower = row_id >= col_id
    ones = jnp.where(lower, 1.0, 0.0).astype(jnp.float32)
    state = s_ref[0]
    for step in range(k_ref.shape[0] // rows):
        here = pl.ds(step * rows, rows)
        cumulative = jnp.dot(
            ones,
            lf_ref[here, :],
            precision=lax.Precision.HIGHEST,
            preferred_element_type=jnp.float32,
        )
        last = cumulative[rows - 1 : rows, :]
        keys = k_ref[here, :]
        values = v_ref[here, :]
        if out_ref is not None:
            centre = cumulative[rows // 2 - 1 : rows // 2, :]
            queries = q_ref[here, :].astype(jnp.float32)
            q_mid = (queries * jnp.exp(cumulative - centre)).astype(jnp.bfloat16)
            k_mid = (keys * jnp.exp(centre - cumulative)).astype(jnp.bfloat16)
            scores = jnp.where(lower, dot_t(q_mid, k_mid, 1, 1), 0.0).astype(jnp.bfloat16)
            raw = dot_t(scores, values, 1, 0) + dot_t(
                (queries * jnp.exp(cumulative)).astype(jnp.bfloat16),
                state.astype(jnp.bfloat16),
                1,
                1,
            )
            scale = lax.rsqrt(jnp.mean(raw * raw, axis=-1, keepdims=True) + NORM_EPS)
            out_ref[here, :] = (raw * scale * gain_ref[...]).astype(jnp.bfloat16)
        k_last = (keys * jnp.exp(last - cumulative)).astype(jnp.bfloat16)
        state = jnp.exp(last) * state + dot_t(values, k_last, 0, 0)
    if state_ref is not None:
        state_ref[0] = state


def recurrence(queries, keys, values, log_forget, state, gain, emit):
    tokens, width = keys.shape
    heads = width // HG_KDIM
    rows = 2 * HG_BLOCK

    def body(q_ref, k_ref, v_ref, lf_ref, s_ref, gain_ref, out_ref):
        recurrence_body(
            rows,
            q_ref,
            k_ref,
            v_ref,
            lf_ref,
            s_ref,
            gain_ref,
            out_ref if emit else None,
            None if emit else out_ref,
        )

    column = pl.BlockSpec((tokens, HG_KDIM), lambda h: (0, h))
    one_state = pl.BlockSpec((1, HG_VDIM, HG_KDIM), lambda h: (h, 0, 0))
    return pl.pallas_call(
        body,
        grid=(heads,),
        in_specs=[
            column,
            column,
            column,
            column,
            one_state,
            pl.BlockSpec((1, HG_VDIM), lambda h: (0, 0)),
        ],
        out_specs=column if emit else one_state,
        out_shape=jax.ShapeDtypeStruct((tokens, width), jnp.bfloat16)
        if emit
        else jax.ShapeDtypeStruct(state.shape, jnp.float32),
        compiler_params=pltpu.CompilerParams(vmem_limit_bytes=32 * 1024 * 1024),
        cost_estimate=pl.CostEstimate(
            flops=tokens * width * 4000, bytes_accessed=tokens * width * 14, transcendentals=0
        ),
        name="rec_out" if emit else "rec_state",
    )(queries, keys, values, log_forget, state, gain)


def attention_body(
    heads, at_ref, q_ref, lat_ref, rope_ref, wk_ref, wv_ref, out_ref, top_ref, tot_ref, acc_ref
):
    step = pl.program_id(0)
    mine = at_ref[0]

    @pl.when(step == 0)
    def _():
        top_ref[...] = jnp.full(top_ref.shape, NEG_BIG, jnp.float32)
        tot_ref[...] = jnp.zeros(tot_ref.shape, jnp.float32)
        acc_ref[...] = jnp.zeros(acc_ref.shape, jnp.float32)

    def visit(masked):
        latent = lat_ref[...]
        rope = rope_ref[...]
        k_all = dot_t(wk_ref[...], latent, 1, 1).astype(jnp.bfloat16)
        v_all = dot_t(wv_ref[...], latent, 1, 1).astype(jnp.bfloat16)
        for head in range(heads):
            k_head = jnp.concatenate([k_all[head * NOPE : (head + 1) * NOPE], rope], axis=0)
            scores = dot_t(k_head, q_ref[head], 0, 0) * (1.0 / math.sqrt(NOPE + ROPE))
            if masked:
                key_id = lax.broadcasted_iota(jnp.int32, scores.shape, 0)
                query_id = lax.broadcasted_iota(jnp.int32, scores.shape, 1)
                scores = jnp.where(key_id <= query_id, scores, NEG_BIG)
            peak = jnp.max(scores, axis=0, keepdims=True)
            weights = jnp.exp(scores - peak)
            total = jnp.sum(weights, axis=0, keepdims=True)
            part = dot_t(
                v_all[head * MLA_V : (head + 1) * MLA_V], weights.astype(jnp.bfloat16), 1, 0
            )
            before = top_ref[head]
            top = jnp.maximum(before, peak)
            old = jnp.exp(before - top)
            new = jnp.exp(peak - top)
            top_ref[head] = top
            tot_ref[head] = tot_ref[head] * old + total * new
            acc_ref[head] = acc_ref[head] * old + part * new

    @pl.when(step < mine)
    def _():
        visit(False)

    @pl.when(step == mine)
    def _():
        visit(True)
        for head in range(heads):
            out_ref[head * MLA_V : (head + 1) * MLA_V, :] = (
                acc_ref[head] / tot_ref[head]
            ).astype(jnp.bfloat16)


def attention(place, queries, latent, rope, w_key, w_value):
    heads, width, rows = queries.shape
    blocks = latent.shape[0] // rows
    grid_spec = pltpu.PrefetchScalarGridSpec(
        num_scalar_prefetch=1,
        grid=(blocks,),
        in_specs=[
            pl.BlockSpec((heads, width, rows), lambda i, at: (0, 0, 0)),
            pl.BlockSpec((rows, latent.shape[1]), lambda i, at: (jnp.minimum(i, at[0]), 0)),
            pl.BlockSpec((rope.shape[0], rows), lambda i, at: (0, jnp.minimum(i, at[0]))),
            pl.BlockSpec(w_key.shape, lambda i, at: (0, 0)),
            pl.BlockSpec(w_value.shape, lambda i, at: (0, 0)),
        ],
        out_specs=pl.BlockSpec((heads * MLA_V, rows), lambda i, at: (0, 0)),
        scratch_shapes=[
            pltpu.VMEM((heads, 1, rows), jnp.float32),
            pltpu.VMEM((heads, 1, rows), jnp.float32),
            pltpu.VMEM((heads, MLA_V, rows), jnp.float32),
        ],
    )

    def body(*refs):
        attention_body(heads, *refs)

    return pl.pallas_call(
        body,
        grid_spec=grid_spec,
        out_shape=jax.ShapeDtypeStruct((heads * MLA_V, rows), jnp.bfloat16),
        compiler_params=pltpu.CompilerParams(
            dimension_semantics=("arbitrary",), vmem_limit_bytes=32 * 1024 * 1024
        ),
        cost_estimate=pl.CostEstimate(
            flops=blocks * heads * rows * rows * 2000,
            bytes_accessed=latent.size * 2,
            transcendentals=0,
        ),
        name="attend",
    )(place, queries, latent, rope, w_key, w_value)


def both_halves(part, axis):
    if lax.axis_size("tp") != 2:
        return lax.all_gather(part, "tp", axis=axis, tiled=True)
    other = lax.ppermute(part, "tp", [(0, 1), (1, 0)])
    first = lax.axis_index("tp") == 0
    return jnp.concatenate(
        [jnp.where(first, part, other), jnp.where(first, other, part)], axis=axis
    )


def shards(
    hidden_in,
    w_query_rec,
    w_forget,
    w_input,
    forget_gap,
    decay_extra,
    rec_gain,
    w_q_down,
    w_kv_down,
    w_key_rope,
    q_gain,
    kv_gain,
    w_q_nope,
    w_q_rope,
    w_k_up,
    w_v_up,
    w_out_rec,
    w_out_att,
):
    tok_dev = hidden_in.shape[0]
    group = lax.axis_size("pl")
    pl_index = lax.axis_index("pl")
    zz_index = lax.axis_index("zz")
    tp_index = lax.axis_index("tp")
    tp_size = lax.axis_size("tp")
    sp_index = zz_index * group + pl_index

    cols = w_query_rec.shape[1] // group
    heads = cols // HG_KDIM
    depth = w_query_rec.shape[0]
    packed = jnp.concatenate(
        [w.reshape(depth, group, cols) for w in (w_query_rec, w_forget, w_input)], axis=2
    )
    swapped = lax.all_to_all(packed, "pl", split_axis=1, concat_axis=0, tiled=True)
    left_weight = lax.all_gather(
        swapped.reshape(group * depth, 3 * cols), "zz", axis=0, tiled=True
    )
    feature_piece = both_halves(hidden_in, 1)
    group_rows = both_halves(lax.all_gather(hidden_in, "pl", axis=0, tiled=True), 1)
    group_decay = lax.all_gather(decay_extra, "pl", axis=0, tiled=True)
    group_decay = lax.dynamic_slice_in_dim(group_decay, pl_index * heads, heads, 1)

    right_weight = jnp.concatenate([w_q_down, w_kv_down, w_key_rope], axis=1)
    right_sum = jnp.dot(feature_piece, right_weight, preferred_element_type=jnp.float32)
    q_cols = w_q_down.shape[1]
    kv_cols = w_kv_down.shape[1]
    right_round = right_sum[:, : q_cols + kv_cols].astype(jnp.bfloat16)
    both = both_halves(right_round[None], 0).astype(jnp.float32)
    q_latent = jnp.concatenate([both[i, :, :q_cols] for i in range(tp_size)], axis=1)
    kv_latent = jnp.concatenate([both[i, :, q_cols:] for i in range(tp_size)], axis=1)
    q_normed = (
        q_latent
        * lax.rsqrt(jnp.mean(q_latent * q_latent, axis=-1, keepdims=True) + NORM_EPS)
        * q_gain
    ).astype(jnp.bfloat16)
    latent = (
        kv_latent
        * lax.rsqrt(jnp.mean(kv_latent * kv_latent, axis=-1, keepdims=True) + NORM_EPS)
        * kv_gain
    ).astype(jnp.bfloat16)
    q_start = sp_index * tok_dev
    cosine, sine_table = rotary_tables(tok_dev, q_start.astype(jnp.float32), ROPE)
    key_rope = rotate_half(right_sum[:, q_cols + kv_cols :], cosine, sine_table).astype(
        jnp.bfloat16
    )
    keys_all = lax.all_gather(
        jnp.concatenate([latent, key_rope], axis=1), ("zz", "pl"), axis=0, tiled=True
    )
    att_heads = w_q_nope.shape[1] // NOPE
    q_nope = jnp.dot(q_normed, w_q_nope, preferred_element_type=jnp.float32).astype(jnp.bfloat16)
    q_rope = jnp.dot(q_normed, w_q_rope, preferred_element_type=jnp.float32).reshape(
        tok_dev, att_heads, ROPE
    )
    q_rope = rotate_half(q_rope, cosine[:, None, :], sine_table[:, None, :]).astype(jnp.bfloat16)
    queries = jnp.concatenate([q_nope.reshape(tok_dev, att_heads, NOPE), q_rope], axis=2)
    att_out = attention(
        sp_index.astype(jnp.int32).reshape(1),
        queries.transpose(1, 2, 0),
        keys_all[:, : latent.shape[1]],
        keys_all[:, latent.shape[1] :].T,
        w_k_up.T,
        w_v_up.T,
    )

    left_round = jnp.dot(
        group_rows, left_weight, preferred_element_type=jnp.float32
    ).astype(jnp.bfloat16)
    rec_query = left_round[:, :cols]
    rec_value = left_round[:, 2 * cols :]
    gap = lax.dynamic_slice_in_dim(forget_gap, pl_index * cols, cols, 0)
    key_in = gap * jax.nn.sigmoid(-left_round[:, cols : 2 * cols].astype(jnp.float32))
    log_forget = jnp.log1p(-key_in) + jnp.repeat(group_decay, HG_KDIM, axis=1)
    gain = rec_gain.reshape(1, HG_VDIM)
    zero_state = jnp.zeros((heads, HG_VDIM, HG_KDIM), jnp.float32)
    local_state = recurrence(rec_query, key_in, rec_value, log_forget, zero_state, gain, False)
    decay = jnp.exp(jnp.sum(log_forget, axis=0)).reshape(heads, 1, HG_KDIM)
    reached = lax.all_gather(jnp.concatenate([local_state, decay], axis=1), "zz", axis=0)
    into_state = zero_state
    for place in range(lax.axis_size("zz") - 1):
        later = reached[place, :, HG_VDIM:] * into_state + reached[place, :, :HG_VDIM]
        into_state = jnp.where(place < zz_index, later, into_state)
    group_out = recurrence(rec_query, key_in, rec_value, log_forget, into_state, gain, True)
    rec_out = lax.all_to_all(group_out, "pl", split_axis=0, concat_axis=1, tiled=True)

    mixed = jnp.dot(rec_out, w_out_rec, preferred_element_type=jnp.float32) + dot_t(
        att_out, w_out_att, 0, 0
    )
    if tp_size != 2:
        return lax.psum_scatter(
            mixed.astype(jnp.bfloat16), "tp", scatter_dimension=0, tiled=True
        )
    half = tok_dev // 2
    sent = lax.dynamic_slice_in_dim(mixed, (1 - tp_index) * half, half, 0).astype(jnp.bfloat16)
    kept = lax.dynamic_slice_in_dim(mixed, tp_index * half, half, 0)
    came = lax.ppermute(sent, "tp", [(0, 1), (1, 0)])
    return (kept + came.astype(jnp.float32)).astype(jnp.bfloat16)


def solution(mesh):
    placed = (
        P(("zz", "pl"), "tp"),
        P(("zz", "pl"), "tp"),
        P(("zz", "pl"), "tp"),
        P(("zz", "pl"), "tp"),
        P("tp"),
        P(("zz", "pl"), "tp"),
        P(),
        P(None, "tp"),
        P(None, "tp"),
        P(),
        P(),
        P(),
        P(None, "tp"),
        P(None, "tp"),
        P(None, "tp"),
        P(None, "tp"),
        P("tp", None),
        P("tp", None),
    )
    sp_size, tp_size = mesh.shape["sp"], mesh.shape["tp"]

    def run(hidden_in, w_query_rec, *rest):
        heads_dev = w_query_rec.shape[1] // HG_KDIM // tp_size
        group = math.gcd(math.gcd(heads_dev, 4), sp_size)
        split_mesh = Mesh(
            mesh.devices.reshape(sp_size // group, group, tp_size), ("zz", "pl", "tp")
        )
        return jax.shard_map(
            shards,
            mesh=split_mesh,
            in_specs=placed,
            out_specs=P(("zz", "pl", "tp"), None),
            check_vma=False,
        )(hidden_in, w_query_rec, *rest)

    return run
```

```python
import math

import jax
import jax.numpy as jnp
from jax import lax
from jax.experimental import pallas as pl
from jax.experimental.pallas import tpu as pltpu
from jax.sharding import Mesh
from jax.sharding import PartitionSpec as P

HG_KDIM = 128
HG_VDIM = 128
HG_BLOCK = 64
NOPE = 64
ROPE = 32
MLA_V = 64


NORM_EPS = 1e-06
ROPE_BASE = 10000.0
NEG_BIG = -1e30


def rotate_half(values, cosine, sine_table):
    half_width = values.shape[-1] // 2
    lower_half = values[..., :half_width]
    upper_half = values[..., half_width:]
    return jnp.concatenate(
        [
            lower_half * cosine - upper_half * sine_table,
            lower_half * sine_table + upper_half * cosine,
        ],
        axis=-1,
    )


def rotary_tables(row_count, offset, rot_width):
    positions = jnp.arange(row_count, dtype=jnp.float32) + offset
    frequency = 1.0 / ROPE_BASE ** (jnp.arange(0, rot_width, 2, dtype=jnp.float32) / rot_width)
    angles = positions[:, None] * frequency[None, :]
    return (jnp.cos(angles), jnp.sin(angles))


def dot_t(left, right, left_dim, right_dim):
    return lax.dot_general(
        left, right, (((left_dim,), (right_dim,)), ((), ())), preferred_element_type=jnp.float32
    )


def recurrence_body(rows, q_ref, k_ref, v_ref, lf_ref, s_ref, gain_ref, out_ref, state_ref):
    row_id = lax.broadcasted_iota(jnp.int32, (rows, rows), 0)
    col_id = lax.broadcasted_iota(jnp.int32, (rows, rows), 1)
    lower = row_id >= col_id
    ones = jnp.where(lower, 1.0, 0.0).astype(jnp.float32)
    state = s_ref[0]
    for step in range(k_ref.shape[0] // rows):
        here = pl.ds(step * rows, rows)
        cumulative = jnp.dot(
            ones,
            lf_ref[here, :],
            precision=lax.Precision.HIGHEST,
            preferred_element_type=jnp.float32,
        )
        last = cumulative[rows - 1 : rows, :]
        keys = k_ref[here, :]
        values = v_ref[here, :]
        if out_ref is not None:
            centre = cumulative[rows // 2 - 1 : rows // 2, :]
            queries = q_ref[here, :].astype(jnp.float32)
            q_mid = (queries * jnp.exp(cumulative - centre)).astype(jnp.bfloat16)
            k_mid = (keys * jnp.exp(centre - cumulative)).astype(jnp.bfloat16)
            scores = jnp.where(lower, dot_t(q_mid, k_mid, 1, 1), 0.0).astype(jnp.bfloat16)
            raw = dot_t(scores, values, 1, 0) + dot_t(
                (queries * jnp.exp(cumulative)).astype(jnp.bfloat16),
                state.astype(jnp.bfloat16),
                1,
                1,
            )
            scale = lax.rsqrt(jnp.mean(raw * raw, axis=-1, keepdims=True) + NORM_EPS)
            out_ref[here, :] = (raw * scale * gain_ref[...]).astype(jnp.bfloat16)
        k_last = (keys * jnp.exp(last - cumulative)).astype(jnp.bfloat16)
        state = jnp.exp(last) * state + dot_t(values, k_last, 0, 0)
    if state_ref is not None:
        state_ref[0] = state


def recurrence(queries, keys, values, log_forget, state, gain, emit):
    tokens, width = keys.shape
    heads = width // HG_KDIM
    rows = 2 * HG_BLOCK

    def body(q_ref, k_ref, v_ref, lf_ref, s_ref, gain_ref, out_ref):
        recurrence_body(
            rows,
            q_ref,
            k_ref,
            v_ref,
            lf_ref,
            s_ref,
            gain_ref,
            out_ref if emit else None,
            None if emit else out_ref,
        )

    column = pl.BlockSpec((tokens, HG_KDIM), lambda h: (0, h))
    one_state = pl.BlockSpec((1, HG_VDIM, HG_KDIM), lambda h: (h, 0, 0))
    return pl.pallas_call(
        body,
        grid=(heads,),
        in_specs=[
            column,
            column,
            column,
            column,
            one_state,
            pl.BlockSpec((1, HG_VDIM), lambda h: (0, 0)),
        ],
        out_specs=column if emit else one_state,
        out_shape=jax.ShapeDtypeStruct((tokens, width), jnp.bfloat16)
        if emit
        else jax.ShapeDtypeStruct(state.shape, jnp.float32),
        compiler_params=pltpu.CompilerParams(vmem_limit_bytes=32 * 1024 * 1024),
        cost_estimate=pl.CostEstimate(
            flops=tokens * width * 4000, bytes_accessed=tokens * width * 14, transcendentals=0
        ),
        name="rec_out" if emit else "rec_state",
    )(queries, keys, values, log_forget, state, gain)


def attention_body(
    heads, at_ref, q_ref, lat_ref, rope_ref, wk_ref, wv_ref, out_ref, top_ref, tot_ref, acc_ref
):
    step = pl.program_id(0)
    mine = at_ref[0]

    @pl.when(step == 0)
    def _():
        top_ref[...] = jnp.full(top_ref.shape, NEG_BIG, jnp.float32)
        tot_ref[...] = jnp.zeros(tot_ref.shape, jnp.float32)
        acc_ref[...] = jnp.zeros(acc_ref.shape, jnp.float32)

    def visit(masked):
        latent = lat_ref[...]
        rope = rope_ref[...]
        k_all = dot_t(wk_ref[...], latent, 1, 1).astype(jnp.bfloat16)
        v_all = dot_t(wv_ref[...], latent, 1, 1).astype(jnp.bfloat16)
        for head in range(heads):
            k_head = jnp.concatenate([k_all[head * NOPE : (head + 1) * NOPE], rope], axis=0)
            scores = dot_t(k_head, q_ref[head], 0, 0) * (1.0 / math.sqrt(NOPE + ROPE))
            if masked:
                key_id = lax.broadcasted_iota(jnp.int32, scores.shape, 0)
                query_id = lax.broadcasted_iota(jnp.int32, scores.shape, 1)
                scores = jnp.where(key_id <= query_id, scores, NEG_BIG)
            peak = jnp.max(scores, axis=0, keepdims=True)
            weights = jnp.exp(scores - peak)
            total = jnp.sum(weights, axis=0, keepdims=True)
            part = dot_t(
                v_all[head * MLA_V : (head + 1) * MLA_V], weights.astype(jnp.bfloat16), 1, 0
            )
            before = top_ref[head]
            top = jnp.maximum(before, peak)
            old = jnp.exp(before - top)
            new = jnp.exp(peak - top)
            top_ref[head] = top
            tot_ref[head] = tot_ref[head] * old + total * new
            acc_ref[head] = acc_ref[head] * old + part * new

    @pl.when(step < mine)
    def _():
        visit(False)

    @pl.when(step == mine)
    def _():
        visit(True)
        for head in range(heads):
            out_ref[head * MLA_V : (head + 1) * MLA_V, :] = (
                acc_ref[head] / tot_ref[head]
            ).astype(jnp.bfloat16)


def attention(place, queries, latent, rope, w_key, w_value):
    heads, width, rows = queries.shape
    blocks = latent.shape[0] // rows
    grid_spec = pltpu.PrefetchScalarGridSpec(
        num_scalar_prefetch=1,
        grid=(blocks,),
        in_specs=[
            pl.BlockSpec((heads, width, rows), lambda i, at: (0, 0, 0)),
            pl.BlockSpec((rows, latent.shape[1]), lambda i, at: (jnp.minimum(i, at[0]), 0)),
            pl.BlockSpec((rope.shape[0], rows), lambda i, at: (0, jnp.minimum(i, at[0]))),
            pl.BlockSpec(w_key.shape, lambda i, at: (0, 0)),
            pl.BlockSpec(w_value.shape, lambda i, at: (0, 0)),
        ],
        out_specs=pl.BlockSpec((heads * MLA_V, rows), lambda i, at: (0, 0)),
        scratch_shapes=[
            pltpu.VMEM((heads, 1, rows), jnp.float32),
            pltpu.VMEM((heads, 1, rows), jnp.float32),
            pltpu.VMEM((heads, MLA_V, rows), jnp.float32),
        ],
    )

    def body(*refs):
        attention_body(heads, *refs)

    return pl.pallas_call(
        body,
        grid_spec=grid_spec,
        out_shape=jax.ShapeDtypeStruct((heads * MLA_V, rows), jnp.bfloat16),
        compiler_params=pltpu.CompilerParams(
            dimension_semantics=("arbitrary",), vmem_limit_bytes=32 * 1024 * 1024
        ),
        cost_estimate=pl.CostEstimate(
            flops=blocks * heads * rows * rows * 2000,
            bytes_accessed=latent.size * 2,
            transcendentals=0,
        ),
        name="attend",
    )(place, queries, latent, rope, w_key, w_value)


def both_halves(part, axis):
    if lax.axis_size("tp") != 2:
        return lax.all_gather(part, "tp", axis=axis, tiled=True)
    other = lax.ppermute(part, "tp", [(0, 1), (1, 0)])
    first = lax.axis_index("tp") == 0
    return jnp.concatenate(
        [jnp.where(first, part, other), jnp.where(first, other, part)], axis=axis
    )


def shards(
    hidden_in,
    w_query_rec,
    w_forget,
    w_input,
    forget_gap,
    decay_extra,
    rec_gain,
    w_q_down,
    w_kv_down,
    w_key_rope,
    q_gain,
    kv_gain,
    w_q_nope,
    w_q_rope,
    w_k_up,
    w_v_up,
    w_out_rec,
    w_out_att,
):
    tok_dev = hidden_in.shape[0]
    group = lax.axis_size("pl")
    pl_index = lax.axis_index("pl")
    zz_index = lax.axis_index("zz")
    tp_index = lax.axis_index("tp")
    tp_size = lax.axis_size("tp")
    sp_index = zz_index * group + pl_index

    cols = w_query_rec.shape[1] // group
    heads = cols // HG_KDIM
    depth = w_query_rec.shape[0]
    packed = jnp.concatenate(
        [w.reshape(depth, group, cols) for w in (w_query_rec, w_forget, w_input)], axis=2
    )
    swapped = lax.all_to_all(packed, "pl", split_axis=1, concat_axis=0, tiled=True)
    left_weight = lax.all_gather(
        swapped.reshape(group * depth, 3 * cols), "zz", axis=0, tiled=True
    )
    feature_piece = both_halves(hidden_in, 1)
    member_rows = [feature_piece]
    for gap_to in range(1, group):
        piece = lax.ppermute(hidden_in, "pl", [(i, i ^ gap_to) for i in range(group)])
        member_rows.append(both_halves(piece, 1))
    group_decay = lax.all_gather(decay_extra, "pl", axis=0, tiled=True)
    group_decay = lax.dynamic_slice_in_dim(group_decay, pl_index * heads, heads, 1)

    right_weight = jnp.concatenate([w_q_down, w_kv_down, w_key_rope], axis=1)
    right_sum = jnp.dot(feature_piece, right_weight, preferred_element_type=jnp.float32)
    q_cols = w_q_down.shape[1]
    kv_cols = w_kv_down.shape[1]
    right_round = right_sum[:, : q_cols + kv_cols].astype(jnp.bfloat16)
    both = both_halves(right_round[None], 0).astype(jnp.float32)
    q_latent = jnp.concatenate([both[i, :, :q_cols] for i in range(tp_size)], axis=1)
    kv_latent = jnp.concatenate([both[i, :, q_cols:] for i in range(tp_size)], axis=1)
    q_normed = (
        q_latent
        * lax.rsqrt(jnp.mean(q_latent * q_latent, axis=-1, keepdims=True) + NORM_EPS)
        * q_gain
    ).astype(jnp.bfloat16)
    latent = (
        kv_latent
        * lax.rsqrt(jnp.mean(kv_latent * kv_latent, axis=-1, keepdims=True) + NORM_EPS)
        * kv_gain
    ).astype(jnp.bfloat16)
    q_start = sp_index * tok_dev
    cosine, sine_table = rotary_tables(tok_dev, q_start.astype(jnp.float32), ROPE)
    key_rope = rotate_half(right_sum[:, q_cols + kv_cols :], cosine, sine_table).astype(
        jnp.bfloat16
    )
    keys_all = lax.all_gather(
        jnp.concatenate([latent, key_rope], axis=1), ("zz", "pl"), axis=0, tiled=True
    )
    att_heads = w_q_nope.shape[1] // NOPE
    q_nope = jnp.dot(q_normed, w_q_nope, preferred_element_type=jnp.float32).astype(jnp.bfloat16)
    q_rope = jnp.dot(q_normed, w_q_rope, preferred_element_type=jnp.float32).reshape(
        tok_dev, att_heads, ROPE
    )
    q_rope = rotate_half(q_rope, cosine[:, None, :], sine_table[:, None, :]).astype(jnp.bfloat16)
    queries = jnp.concatenate([q_nope.reshape(tok_dev, att_heads, NOPE), q_rope], axis=2)
    att_out = attention(
        sp_index.astype(jnp.int32).reshape(1),
        queries.transpose(1, 2, 0),
        keys_all[:, : latent.shape[1]],
        keys_all[:, latent.shape[1] :].T,
        w_k_up.T,
        w_v_up.T,
    )

    left_weight, att_out = lax.optimization_barrier((left_weight, att_out))
    left_round = jnp.zeros((group * tok_dev, 3 * cols), jnp.bfloat16)
    for gap_to, rows in enumerate(member_rows):
        projected = jnp.dot(rows, left_weight, preferred_element_type=jnp.float32)
        left_round = lax.dynamic_update_slice_in_dim(
            left_round, projected.astype(jnp.bfloat16), (pl_index ^ gap_to) * tok_dev, 0
        )
    rec_query = left_round[:, :cols]
    rec_value = left_round[:, 2 * cols :]
    gap = lax.dynamic_slice_in_dim(forget_gap, pl_index * cols, cols, 0)
    key_in = gap * jax.nn.sigmoid(-left_round[:, cols : 2 * cols].astype(jnp.float32))
    log_forget = jnp.log1p(-key_in) + jnp.repeat(group_decay, HG_KDIM, axis=1)
    gain = rec_gain.reshape(1, HG_VDIM)
    zero_state = jnp.zeros((heads, HG_VDIM, HG_KDIM), jnp.float32)
    local_state = recurrence(rec_query, key_in, rec_value, log_forget, zero_state, gain, False)
    decay = jnp.exp(jnp.sum(log_forget, axis=0)).reshape(heads, 1, HG_KDIM)
    reached = jnp.concatenate([local_state, decay], axis=1)
    zz_size = lax.axis_size("zz")
    into_state = zero_state
    if zz_size <= 4:
        for back in range(zz_size - 1, 0, -1):
            came = lax.ppermute(reached, "zz", [(i, i + back) for i in range(zz_size - back)])
            into_state = came[:, HG_VDIM:] * into_state + came[:, :HG_VDIM]
    else:
        reached = lax.all_gather(reached, "zz", axis=0)
        for place in range(zz_size - 1):
            later = reached[place, :, HG_VDIM:] * into_state + reached[place, :, :HG_VDIM]
            into_state = jnp.where(place < zz_index, later, into_state)
    group_out = recurrence(rec_query, key_in, rec_value, log_forget, into_state, gain, True)
    rec_out = lax.all_to_all(group_out, "pl", split_axis=0, concat_axis=1, tiled=True)

    mixed = jnp.dot(rec_out, w_out_rec, preferred_element_type=jnp.float32) + dot_t(
        att_out, w_out_att, 0, 0
    )
    if tp_size != 2:
        return lax.psum_scatter(
            mixed.astype(jnp.bfloat16), "tp", scatter_dimension=0, tiled=True
        )
    half = tok_dev // 2
    sent = lax.dynamic_slice_in_dim(mixed, (1 - tp_index) * half, half, 0).astype(jnp.bfloat16)
    kept = lax.dynamic_slice_in_dim(mixed, tp_index * half, half, 0)
    came = lax.ppermute(sent, "tp", [(0, 1), (1, 0)])
    return (kept + came.astype(jnp.float32)).astype(jnp.bfloat16)


def solution(mesh):
    placed = (
        P(("zz", "pl"), "tp"),
        P(("zz", "pl"), "tp"),
        P(("zz", "pl"), "tp"),
        P(("zz", "pl"), "tp"),
        P("tp"),
        P(("zz", "pl"), "tp"),
        P(),
        P(None, "tp"),
        P(None, "tp"),
        P(),
        P(),
        P(),
        P(None, "tp"),
        P(None, "tp"),
        P(None, "tp"),
        P(None, "tp"),
        P("tp", None),
        P("tp", None),
    )
    sp_size, tp_size = mesh.shape["sp"], mesh.shape["tp"]

    def run(hidden_in, w_query_rec, *rest):
        heads_dev = w_query_rec.shape[1] // HG_KDIM // tp_size
        group = math.gcd(math.gcd(heads_dev, 4), sp_size)
        split_mesh = Mesh(
            mesh.devices.reshape(sp_size // group, group, tp_size), ("zz", "pl", "tp")
        )
        return jax.shard_map(
            shards,
            mesh=split_mesh,
            in_specs=placed,
            out_specs=P(("zz", "pl", "tp"), None),
            check_vma=False,
        )(hidden_in, w_query_rec, *rest)

    return run
```

```python
import math

import jax
import jax.numpy as jnp
from jax import lax
from jax.experimental import pallas as pl
from jax.experimental.pallas import tpu as pltpu
from jax.sharding import Mesh
from jax.sharding import PartitionSpec as P

HG_KDIM = 128
HG_VDIM = 128
HG_BLOCK = 64
NOPE = 64
ROPE = 32
MLA_V = 64


NORM_EPS = 1e-06
ROPE_BASE = 10000.0
NEG_BIG = -1e30


def rotate_half(values, cosine, sine_table):
    half_width = values.shape[-1] // 2
    lower_half = values[..., :half_width]
    upper_half = values[..., half_width:]
    return jnp.concatenate(
        [
            lower_half * cosine - upper_half * sine_table,
            lower_half * sine_table + upper_half * cosine,
        ],
        axis=-1,
    )


def rotary_tables(row_count, offset, rot_width):
    positions = jnp.arange(row_count, dtype=jnp.float32) + offset
    frequency = 1.0 / ROPE_BASE ** (jnp.arange(0, rot_width, 2, dtype=jnp.float32) / rot_width)
    angles = positions[:, None] * frequency[None, :]
    return (jnp.cos(angles), jnp.sin(angles))


def dot_t(left, right, left_dim, right_dim):
    return lax.dot_general(
        left, right, (((left_dim,), (right_dim,)), ((), ())), preferred_element_type=jnp.float32
    )


def recurrence_body(rows, q_ref, k_ref, v_ref, lf_ref, s_ref, gain_ref, out_ref, state_ref):
    row_id = lax.broadcasted_iota(jnp.int32, (rows, rows), 0)
    col_id = lax.broadcasted_iota(jnp.int32, (rows, rows), 1)
    lower = row_id >= col_id
    ones = jnp.where(lower, 1.0, 0.0).astype(jnp.float32)
    state = s_ref[0]
    for step in range(k_ref.shape[0] // rows):
        here = pl.ds(step * rows, rows)
        cumulative = jnp.dot(
            ones,
            lf_ref[here, :],
            precision=lax.Precision.HIGHEST,
            preferred_element_type=jnp.float32,
        )
        last = cumulative[rows - 1 : rows, :]
        keys = k_ref[here, :]
        values = v_ref[here, :]
        if out_ref is not None:
            centre = cumulative[rows // 2 - 1 : rows // 2, :]
            queries = q_ref[here, :].astype(jnp.float32)
            q_mid = (queries * jnp.exp(cumulative - centre)).astype(jnp.bfloat16)
            k_mid = (keys * jnp.exp(centre - cumulative)).astype(jnp.bfloat16)
            scores = jnp.where(lower, dot_t(q_mid, k_mid, 1, 1), 0.0).astype(jnp.bfloat16)
            raw = dot_t(scores, values, 1, 0) + dot_t(
                (queries * jnp.exp(cumulative)).astype(jnp.bfloat16),
                state.astype(jnp.bfloat16),
                1,
                1,
            )
            scale = lax.rsqrt(jnp.mean(raw * raw, axis=-1, keepdims=True) + NORM_EPS)
            out_ref[here, :] = (raw * scale * gain_ref[...]).astype(jnp.bfloat16)
        k_last = (keys * jnp.exp(last - cumulative)).astype(jnp.bfloat16)
        state = jnp.exp(last) * state + dot_t(values, k_last, 0, 0)
    if state_ref is not None:
        state_ref[0] = state


def recurrence(queries, keys, values, log_forget, state, gain, emit):
    tokens, width = keys.shape
    heads = width // HG_KDIM
    rows = 2 * HG_BLOCK

    def body(q_ref, k_ref, v_ref, lf_ref, s_ref, gain_ref, out_ref):
        recurrence_body(
            rows,
            q_ref,
            k_ref,
            v_ref,
            lf_ref,
            s_ref,
            gain_ref,
            out_ref if emit else None,
            None if emit else out_ref,
        )

    column = pl.BlockSpec((tokens, HG_KDIM), lambda h: (0, h))
    one_state = pl.BlockSpec((1, HG_VDIM, HG_KDIM), lambda h: (h, 0, 0))
    return pl.pallas_call(
        body,
        grid=(heads,),
        in_specs=[
            column,
            column,
            column,
            column,
            one_state,
            pl.BlockSpec((1, HG_VDIM), lambda h: (0, 0)),
        ],
        out_specs=column if emit else one_state,
        out_shape=jax.ShapeDtypeStruct((tokens, width), jnp.bfloat16)
        if emit
        else jax.ShapeDtypeStruct(state.shape, jnp.float32),
        compiler_params=pltpu.CompilerParams(vmem_limit_bytes=32 * 1024 * 1024),
        cost_estimate=pl.CostEstimate(
            flops=tokens * width * 4000, bytes_accessed=tokens * width * 14, transcendentals=0
        ),
        name="rec_out" if emit else "rec_state",
    )(queries, keys, values, log_forget, state, gain)


def attention_body(
    heads, at_ref, q_ref, lat_ref, rope_ref, wk_ref, wv_ref, out_ref, top_ref, tot_ref, acc_ref
):
    step = pl.program_id(0)
    mine = at_ref[0]

    @pl.when(step == 0)
    def _():
        top_ref[...] = jnp.full(top_ref.shape, NEG_BIG, jnp.float32)
        tot_ref[...] = jnp.zeros(tot_ref.shape, jnp.float32)
        acc_ref[...] = jnp.zeros(acc_ref.shape, jnp.float32)

    def visit(masked):
        latent = lat_ref[...]
        rope = rope_ref[...]
        k_all = dot_t(wk_ref[...], latent, 1, 1).astype(jnp.bfloat16)
        v_all = dot_t(wv_ref[...], latent, 1, 1).astype(jnp.bfloat16)
        for head in range(heads):
            k_head = jnp.concatenate([k_all[head * NOPE : (head + 1) * NOPE], rope], axis=0)
            scores = dot_t(k_head, q_ref[head], 0, 0) * (1.0 / math.sqrt(NOPE + ROPE))
            if masked:
                key_id = lax.broadcasted_iota(jnp.int32, scores.shape, 0)
                query_id = lax.broadcasted_iota(jnp.int32, scores.shape, 1)
                scores = jnp.where(key_id <= query_id, scores, NEG_BIG)
            peak = jnp.max(scores, axis=0, keepdims=True)
            weights = jnp.exp(scores - peak)
            total = jnp.sum(weights, axis=0, keepdims=True)
            part = dot_t(
                v_all[head * MLA_V : (head + 1) * MLA_V], weights.astype(jnp.bfloat16), 1, 0
            )
            before = top_ref[head]
            top = jnp.maximum(before, peak)
            old = jnp.exp(before - top)
            new = jnp.exp(peak - top)
            top_ref[head] = top
            tot_ref[head] = tot_ref[head] * old + total * new
            acc_ref[head] = acc_ref[head] * old + part * new

    @pl.when(step < mine)
    def _():
        visit(False)

    @pl.when(step == mine)
    def _():
        visit(True)
        for head in range(heads):
            out_ref[head * MLA_V : (head + 1) * MLA_V, :] = (
                acc_ref[head] / tot_ref[head]
            ).astype(jnp.bfloat16)


def attention(place, queries, latent, rope, w_key, w_value):
    heads, width, rows = queries.shape
    blocks = latent.shape[0] // rows
    grid_spec = pltpu.PrefetchScalarGridSpec(
        num_scalar_prefetch=1,
        grid=(blocks,),
        in_specs=[
            pl.BlockSpec((heads, width, rows), lambda i, at: (0, 0, 0)),
            pl.BlockSpec((rows, latent.shape[1]), lambda i, at: (jnp.minimum(i, at[0]), 0)),
            pl.BlockSpec((rope.shape[0], rows), lambda i, at: (0, jnp.minimum(i, at[0]))),
            pl.BlockSpec(w_key.shape, lambda i, at: (0, 0)),
            pl.BlockSpec(w_value.shape, lambda i, at: (0, 0)),
        ],
        out_specs=pl.BlockSpec((heads * MLA_V, rows), lambda i, at: (0, 0)),
        scratch_shapes=[
            pltpu.VMEM((heads, 1, rows), jnp.float32),
            pltpu.VMEM((heads, 1, rows), jnp.float32),
            pltpu.VMEM((heads, MLA_V, rows), jnp.float32),
        ],
    )

    def body(*refs):
        attention_body(heads, *refs)

    return pl.pallas_call(
        body,
        grid_spec=grid_spec,
        out_shape=jax.ShapeDtypeStruct((heads * MLA_V, rows), jnp.bfloat16),
        compiler_params=pltpu.CompilerParams(
            dimension_semantics=("arbitrary",), vmem_limit_bytes=32 * 1024 * 1024
        ),
        cost_estimate=pl.CostEstimate(
            flops=blocks * heads * rows * rows * 2000,
            bytes_accessed=latent.size * 2,
            transcendentals=0,
        ),
        name="attend",
    )(place, queries, latent, rope, w_key, w_value)


def both_halves(part, axis):
    if lax.axis_size("tp") != 2:
        return lax.all_gather(part, "tp", axis=axis, tiled=True)
    other = lax.ppermute(part, "tp", [(0, 1), (1, 0)])
    first = lax.axis_index("tp") == 0
    return jnp.concatenate(
        [jnp.where(first, part, other), jnp.where(first, other, part)], axis=axis
    )


def shards(
    hidden_in,
    w_query_rec,
    w_forget,
    w_input,
    forget_gap,
    decay_extra,
    rec_gain,
    w_q_down,
    w_kv_down,
    w_key_rope,
    q_gain,
    kv_gain,
    w_q_nope,
    w_q_rope,
    w_k_up,
    w_v_up,
    w_out_rec,
    w_out_att,
):
    tok_dev = hidden_in.shape[0]
    group = lax.axis_size("pl")
    pl_index = lax.axis_index("pl")
    zz_index = lax.axis_index("zz")
    tp_index = lax.axis_index("tp")
    tp_size = lax.axis_size("tp")
    sp_index = zz_index * group + pl_index

    cols = w_query_rec.shape[1] // group
    heads = cols // HG_KDIM
    depth = w_query_rec.shape[0]
    packed = jnp.concatenate(
        [w.reshape(depth, group, cols) for w in (w_query_rec, w_forget, w_input)], axis=2
    )
    swapped = lax.all_to_all(packed, "pl", split_axis=1, concat_axis=0, tiled=True)
    left_weight = lax.all_gather(
        swapped.reshape(group * depth, 3 * cols), "zz", axis=0, tiled=True
    )
    feature_piece = both_halves(hidden_in, 1)
    member_rows = [feature_piece]
    for gap_to in range(1, group):
        piece = lax.ppermute(hidden_in, "pl", [(i, i ^ gap_to) for i in range(group)])
        member_rows.append(both_halves(piece, 1))
    group_decay = lax.all_gather(decay_extra, "pl", axis=0, tiled=True)
    group_decay = lax.dynamic_slice_in_dim(group_decay, pl_index * heads, heads, 1)

    right_weight = jnp.concatenate([w_q_down, w_kv_down, w_key_rope], axis=1)
    right_sum = jnp.dot(feature_piece, right_weight, preferred_element_type=jnp.float32)
    q_cols = w_q_down.shape[1]
    kv_cols = w_kv_down.shape[1]
    right_round = right_sum[:, : q_cols + kv_cols].astype(jnp.bfloat16)
    both = both_halves(right_round[None], 0).astype(jnp.float32)
    q_latent = jnp.concatenate([both[i, :, :q_cols] for i in range(tp_size)], axis=1)
    kv_latent = jnp.concatenate([both[i, :, q_cols:] for i in range(tp_size)], axis=1)
    q_normed = (
        q_latent
        * lax.rsqrt(jnp.mean(q_latent * q_latent, axis=-1, keepdims=True) + NORM_EPS)
        * q_gain
    ).astype(jnp.bfloat16)
    latent = (
        kv_latent
        * lax.rsqrt(jnp.mean(kv_latent * kv_latent, axis=-1, keepdims=True) + NORM_EPS)
        * kv_gain
    ).astype(jnp.bfloat16)
    q_start = sp_index * tok_dev
    cosine, sine_table = rotary_tables(tok_dev, q_start.astype(jnp.float32), ROPE)
    key_rope = rotate_half(right_sum[:, q_cols + kv_cols :], cosine, sine_table).astype(
        jnp.bfloat16
    )
    group_keys = lax.all_gather(
        jnp.concatenate([latent, key_rope], axis=1), "pl", axis=0, tiled=True
    )
    keys_all = lax.all_gather(group_keys, "zz", axis=0, tiled=True)
    att_heads = w_q_nope.shape[1] // NOPE
    q_nope = jnp.dot(q_normed, w_q_nope, preferred_element_type=jnp.float32).astype(jnp.bfloat16)
    q_rope = jnp.dot(q_normed, w_q_rope, preferred_element_type=jnp.float32).reshape(
        tok_dev, att_heads, ROPE
    )
    q_rope = rotate_half(q_rope, cosine[:, None, :], sine_table[:, None, :]).astype(jnp.bfloat16)
    queries = jnp.concatenate([q_nope.reshape(tok_dev, att_heads, NOPE), q_rope], axis=2)
    att_out = attention(
        sp_index.astype(jnp.int32).reshape(1),
        queries.transpose(1, 2, 0),
        keys_all[:, : latent.shape[1]],
        keys_all[:, latent.shape[1] :].T,
        w_k_up.T,
        w_v_up.T,
    )

    left_weight, att_out = lax.optimization_barrier((left_weight, att_out))
    left_round = jnp.zeros((group * tok_dev, 3 * cols), jnp.bfloat16)
    for gap_to, rows in enumerate(member_rows):
        projected = jnp.dot(rows, left_weight, preferred_element_type=jnp.float32)
        left_round = lax.dynamic_update_slice_in_dim(
            left_round, projected.astype(jnp.bfloat16), (pl_index ^ gap_to) * tok_dev, 0
        )
    rec_query = left_round[:, :cols]
    rec_value = left_round[:, 2 * cols :]
    gap = lax.dynamic_slice_in_dim(forget_gap, pl_index * cols, cols, 0)
    key_in = gap * jax.nn.sigmoid(-left_round[:, cols : 2 * cols].astype(jnp.float32))
    log_forget = jnp.log1p(-key_in) + jnp.repeat(group_decay, HG_KDIM, axis=1)
    gain = rec_gain.reshape(1, HG_VDIM)
    zero_state = jnp.zeros((heads, HG_VDIM, HG_KDIM), jnp.float32)
    local_state = recurrence(rec_query, key_in, rec_value, log_forget, zero_state, gain, False)
    decay = jnp.exp(jnp.sum(log_forget, axis=0)).reshape(heads, 1, HG_KDIM)
    reached = jnp.concatenate([local_state, decay], axis=1)
    zz_size = lax.axis_size("zz")
    into_state = zero_state
    if zz_size <= 4:
        for back in range(zz_size - 1, 0, -1):
            came = lax.ppermute(reached, "zz", [(i, i + back) for i in range(zz_size - back)])
            into_state = came[:, HG_VDIM:] * into_state + came[:, :HG_VDIM]
    else:
        reached = lax.all_gather(reached, "zz", axis=0)
        for place in range(zz_size - 1):
            later = reached[place, :, HG_VDIM:] * into_state + reached[place, :, :HG_VDIM]
            into_state = jnp.where(place < zz_index, later, into_state)
    group_out = recurrence(rec_query, key_in, rec_value, log_forget, into_state, gain, True)
    rec_out = lax.all_to_all(group_out, "pl", split_axis=0, concat_axis=1, tiled=True)

    mixed = jnp.dot(rec_out, w_out_rec, preferred_element_type=jnp.float32) + dot_t(
        att_out, w_out_att, 0, 0
    )
    if tp_size != 2:
        return lax.psum_scatter(
            mixed.astype(jnp.bfloat16), "tp", scatter_dimension=0, tiled=True
        )
    half = tok_dev // 2
    sent = lax.dynamic_slice_in_dim(mixed, (1 - tp_index) * half, half, 0).astype(jnp.bfloat16)
    kept = lax.dynamic_slice_in_dim(mixed, tp_index * half, half, 0)
    came = lax.ppermute(sent, "tp", [(0, 1), (1, 0)])
    return (kept + came.astype(jnp.float32)).astype(jnp.bfloat16)


def solution(mesh):
    placed = (
        P(("zz", "pl"), "tp"),
        P(("zz", "pl"), "tp"),
        P(("zz", "pl"), "tp"),
        P(("zz", "pl"), "tp"),
        P("tp"),
        P(("zz", "pl"), "tp"),
        P(),
        P(None, "tp"),
        P(None, "tp"),
        P(),
        P(),
        P(),
        P(None, "tp"),
        P(None, "tp"),
        P(None, "tp"),
        P(None, "tp"),
        P("tp", None),
        P("tp", None),
    )
    sp_size, tp_size = mesh.shape["sp"], mesh.shape["tp"]

    def run(hidden_in, w_query_rec, *rest):
        heads_dev = w_query_rec.shape[1] // HG_KDIM // tp_size
        group = math.gcd(math.gcd(heads_dev, 4), sp_size)
        split_mesh = Mesh(
            mesh.devices.reshape(sp_size // group, group, tp_size), ("zz", "pl", "tp")
        )
        return jax.shard_map(
            shards,
            mesh=split_mesh,
            in_specs=placed,
            out_specs=P(("zz", "pl", "tp"), None),
            check_vma=False,
        )(hidden_in, w_query_rec, *rest)

    return run
```
